32 devices in a mesh: sp: 8 (over z, core), tp: 4 (over y, x).
Axes of the slice: x: 2, y: 2, z: 4, core: 2. Of those that a mesh axis runs over, the one named last changes fastest.
Arguments:
- queries: bfloat16 [4096, 1024], P('sp', 'tp'), may hold values from -20 to 20
- key_vectors: bfloat16 [4096, 1024], P('sp', 'tp'), may hold values from -20 to 20
- value_vectors: bfloat16 [4096, 1024], P('sp', 'tp'), may hold values from -6 to 6
- log_gate_sums: float32 [4096, 16], P('sp', 'tp'), may hold values from -588 to 0, as said below
- residual: bfloat16 [4096, 2048], P('sp', 'tp'), may hold values from -24 to 24
- out_weight: bfloat16 [1024, 2048], P(None, 'tp'), may hold values from -0.75 to 0.75
- norm_gain: bfloat16 [2048], replicated, may hold values from 0.099609375 to 1.8984375
- routes: int32 [4096, 2], P('sp'), may hold values from 0 to 31, all different within a row; in each aligned block of 512 rows (0 to 511, 512 to 1023, ...) at most 40 rows name the same one
- route_weight: float32 [4096, 2], P('sp'), may hold values from 0.5 to 1.5
- expert_gate: bfloat16 [32, 2048, 512], P('sp', None, 'tp'), may hold values from -0.125 to 0.125
- expert_up: bfloat16 [32, 2048, 512], P('sp', None, 'tp'), may hold values from -0.125 to 0.125
- expert_down: bfloat16 [32, 512, 2048], P('sp', None, 'tp'), may hold values from -0.25 to 0.25
- shared_gate: bfloat16 [2048, 512], P(None, 'tp'), may hold values from -0.125 to 0.125
- shared_up: bfloat16 [2048, 512], P(None, 'tp'), may hold values from -0.125 to 0.125
- shared_down: bfloat16 [512, 2048], P(None, 'tp'), may hold values from -0.25 to 0.25
Outputs:
- layer_out: bfloat16 [4096, 2048], P('sp', 'tp')
The draws below stay inside these ranges and needn't reach their ends.
Inputs may be any that keep to these rules, and one draw needn't show every extreme that they name: `log_gate_sums`: for each head the values do not rise along the positions. `routes`: each row names 2 different experts; among the rows of one index of sp no expert is named by more than 40 rows, a bound that some block reaches.
All inputs are finite; a program needn't handle non-finite values.
Results may differ from the reference program's by a relative error of at most 0.014.
Values may be sent and summed in bfloat16 or wider, within the bound.
A program may use at most 64 MiB of HBM per device.

```python
import math
import jax
import jax.numpy as jnp
import numpy as np
from jax import lax

D = 2048
HEAD_TOTAL = 16
HDIM = 64
EF = 512
SH = 512
TOPK = 2
TOK_DEV = 512
TOKEN_TOTAL = 4096
EXPERTS = 32
CAP = 40
N_SP = 8


def attention_pair(key):
    base_key = jax.random.fold_in(key, 11)
    key_query, key_keys = jax.random.split(base_key, 2)
    width = HEAD_TOTAL * HDIM
    query_draw = 1.5 * jax.random.normal(key_query, (TOKEN_TOTAL, width), jnp.float32)
    key_draw = 1.5 * jax.random.normal(key_keys, (TOKEN_TOTAL, width), jnp.float32)
    return (jnp.clip(query_draw, -20.0, 20.0), jnp.clip(key_draw, -20.0, 20.0))


def draw_queries(key, part):
    return attention_pair(key)[0].astype(jnp.bfloat16)


def draw_key_vectors(key, part):
    return attention_pair(key)[1].astype(jnp.bfloat16)


def draw_log_gate_sums(key, part):
    key_a, key_b, key_c, random_key_fourth, random_key_fifth = jax.random.split(jax.random.fold_in(key, 23), 5)
    keep_share = 0.5
    slower_decay_heads = jax.random.bernoulli(key_a, keep_share, (HEAD_TOTAL,))
    rate = jnp.where(slower_decay_heads, 0.4 / TOKEN_TOTAL, 1.0 / 40.0)
    block_factor = 2.0 ** jax.random.uniform(key_b, (TOKEN_TOTAL // TOK_DEV, 1), jnp.float32, -1.0, 1.0)
    per_token = jnp.repeat(block_factor, TOK_DEV, axis=0)
    data_factor = jnp.exp(jax.random.uniform(key_c, (TOKEN_TOTAL, HEAD_TOTAL), jnp.float32, -1.0, 1.0))
    logarithm_decay_terms = -rate[None, :] * per_token * data_factor
    cluster_positions = jax.random.randint(random_key_fourth, (3,), 0, TOKEN_TOTAL)
    cluster_length = jnp.log(jax.random.uniform(random_key_fifth, (3, HEAD_TOTAL), jnp.float32, 0.5, 0.8))
    cluster_token_count = (jnp.arange(TOKEN_TOTAL, dtype=jnp.int32)[:, None] == cluster_positions[None, :]).astype(jnp.float32)
    token_clusters = jnp.sum(cluster_token_count[:, :, None] * cluster_length[None, :, :], axis=1)
    logarithm_decay_terms = logarithm_decay_terms + jnp.where(slower_decay_heads[None, :], token_clusters, 0.0)
    return jnp.cumsum(logarithm_decay_terms, axis=0)


def draw_residual(key, part):
    key_a = jax.random.fold_in(jax.random.fold_in(key, 31), 0)
    key_c = jax.random.fold_in(jax.random.fold_in(key, 31), 2)
    column = jnp.arange(D, dtype=jnp.float32) / D
    base_draw = jax.random.normal(key_a, (TOKEN_TOTAL, D), jnp.float32)
    col_scale = 0.4 * 5.0 ** column * jax.random.uniform(key_c, (D,), jnp.float32, 0.7, 1.3)
    values = col_scale[None, :] * base_draw
    return jnp.clip(values, -24.0, 24.0).astype(jnp.bfloat16)


def block_scale(key, extent, shards, least, top_value):
    loudness = 1.0
    for axis_at, parts in shards:
        draws = jax.random.uniform(jax.random.fold_in(jax.random.fold_in(key, 6), axis_at), (parts,), jnp.float32, least / len(shards), top_value / len(shards))
        loudness = loudness * jnp.repeat(jnp.exp(draws), extent[axis_at] // parts).reshape((-1,) + (1,) * (len(extent) - 1 - axis_at))
    return loudness


def deal_out(stream_key, own, number, rows, amount, top, bound, lean):
    ranking = jax.random.permutation(stream_key, amount)
    packed, common = portions_of(amount, rows * top, bound, lean, True), portions_of(amount, rows * top, bound, lean, False)
    places = jnp.arange(amount)

    def named(lengths, rotation):
        used = int((lengths > 0).sum())
        fixed = max(1, used // 4)
        shifted = fixed + (places - fixed + rotation * (used - fixed)) % max(1, amount - fixed)
        return jnp.zeros((amount,), jnp.int32).at[ranking[jnp.where(places < fixed, places, shifted)]].set(jnp.asarray(lengths, jnp.int32))

    lengths = jnp.where(number % 4 == 0, named(packed, number // 4), named(common, number - number // 4 - 1))
    mixed = jax.random.permutation(jax.random.fold_in(own, 3), amount)
    donor, sink = mixed[0:amount // 2 * 2:2], mixed[1:amount // 2 * 2:2]
    slack = jnp.minimum(lengths[donor] - 1, bound - lengths[sink]) // 2
    slack = jnp.where((donor == ranking[0]) | (sink == ranking[0]) | (lengths[sink] == 0), 0, jnp.maximum(slack, 0))
    shifted = jax.random.randint(jax.random.fold_in(own, 4), (amount // 2,), 0, 1 << 20) % (slack + 1)
    lengths = lengths.at[donor].add(-shifted).at[sink].add(shifted)
    members = jnp.searchsorted(jnp.cumsum(lengths), jnp.arange(rows * top), side="right").astype(jnp.int32)
    grid = members.reshape(top, rows).T
    grid = grid[jax.random.permutation(jax.random.fold_in(own, 1), rows)]
    rotation = jax.random.randint(jax.random.fold_in(own, 2), (rows, 1), 0, top)
    return jnp.take_along_axis(grid, (jnp.arange(top)[None, :] + rotation) % top, axis=1)


def portions_of(count, total, limit, lean, full):
    loads = [(1 << 20) // math.isqrt(grade ** lean) + 1 for grade in range(1, count + 1)]
    largest = limit if full else min(limit, max(-(-total // count), total * loads[0] // sum(loads)))
    least = 1 if total - largest >= count - 1 else 0
    counts, rest = [largest] + [least] * (count - 1), total - largest - least * (count - 1)
    while rest > 0:
        free = [i for i in range(1, count) if counts[i] < largest] or [i for i in range(1, count) if counts[i] < limit]
        mass, budget = sum([loads[i] for i in free]), rest
        for i in free:
            extra = min(limit - counts[i], max(1, budget * loads[i] // mass), rest)
            counts[i] = counts[i] + extra
            rest = rest - extra
    return np.array(counts)


def normal_values(rng, extent, deviation, bound, pieces=(), kind=jnp.bfloat16):
    loudness = block_scale(rng, extent, pieces, -0.22, 0.18) if pieces else 1.0
    entries = jax.random.normal(rng, extent, jnp.float32) * deviation * loudness
    return jnp.minimum(jnp.maximum(entries, -bound), bound).astype(kind)


def setup_inputs(seed: int = 0) -> dict:
    keys = jax.random.split(jax.random.key(seed), 16)
    queries = draw_queries(jax.random.fold_in(keys[15], 71), 0)
    key_vectors = draw_key_vectors(jax.random.fold_in(keys[15], 71), 0)
    value_vectors = normal_values(keys[2], (TOKEN_TOTAL, HEAD_TOTAL * HDIM), 1.0, 6.0, ((0, 8), (1, 4)))
    log_gate_sums = draw_log_gate_sums(jax.random.fold_in(keys[15], 71), 0)
    residual = draw_residual(jax.random.fold_in(keys[15], 71), 0)
    out_weight = normal_values(keys[5], (HEAD_TOTAL * HDIM, D), (HEAD_TOTAL * HDIM // 16) ** -0.5, 0.75, ((1, 4),))
    norm_gain = jnp.clip(1.0 + 0.18 * jax.random.normal(keys[6], (D,), jnp.float32), 0.099609375, 1.8984375).astype(jnp.bfloat16)
    routes_keys = jax.random.split(jax.random.fold_in(keys[7], 1), TOKEN_TOTAL // TOK_DEV)
    routes_turns = jax.random.permutation(jax.random.fold_in(keys[7], 3), TOKEN_TOTAL // TOK_DEV)
    routes = jax.vmap(lambda own, number: deal_out(jax.random.fold_in(keys[7], 2), own, number, TOK_DEV, EXPERTS, TOPK, CAP, 1))(routes_keys, routes_turns).reshape((TOKEN_TOTAL, TOPK))
    route_weight = jnp.clip(0.5 + 1.0 * jax.random.uniform(keys[8], (TOKEN_TOTAL, TOPK), jnp.float32) ** block_scale(keys[8], (TOKEN_TOTAL, TOPK), ((0, 8),), -0.2, 0.2), 0.5, 1.5)
    expert_gate = normal_values(keys[9], (EXPERTS, D, EF), D ** -0.5, 0.125, ((0, 8), (2, 4)))
    expert_up = normal_values(keys[10], (EXPERTS, D, EF), D ** -0.5, 0.125, ((0, 8), (2, 4)))
    expert_down = normal_values(keys[11], (EXPERTS, EF, D), EF ** -0.5, 0.25, ((0, 8), (2, 4)))
    shared_gate = normal_values(keys[12], (D, SH), D ** -0.5, 0.125, ((1, 4),))
    shared_up = normal_values(keys[13], (D, SH), D ** -0.5, 0.125, ((1, 4),))
    shared_down = normal_values(keys[14], (SH, D), SH ** -0.5, 0.25, ((1, 4),))
    return dict(queries=queries, key_vectors=key_vectors, value_vectors=value_vectors, log_gate_sums=log_gate_sums, residual=residual, out_weight=out_weight, norm_gain=norm_gain, routes=routes, route_weight=route_weight, expert_gate=expert_gate, expert_up=expert_up, expert_down=expert_down, shared_gate=shared_gate, shared_up=shared_up, shared_down=shared_down)


EPSILON = 1e-06

def silu_gate(gate_part, up_part):
    return jax.nn.silu(gate_part) * up_part

def one_head(inputs):
    query_head, key_head, value_head, gate_head = inputs
    block_size = math.gcd(TOKEN_TOTAL, 512)
    key_pos = jnp.arange(TOKEN_TOTAL, dtype=jnp.int32)
    score_scale = HDIM ** (-0.5)

    def one_block(block_number):
        first_row = (block_number * block_size).astype(jnp.int32)
        query_block = lax.dynamic_slice_in_dim(query_head, first_row, block_size, 0)
        gate_block = lax.dynamic_slice_in_dim(gate_head, first_row, block_size, 0)
        scores = jnp.dot(query_block, key_head.T, preferred_element_type=jnp.float32) * score_scale
        scores = scores + gate_block[:, None] - gate_head[None, :]
        query_pos = first_row + jnp.arange(block_size, dtype=jnp.int32)
        allowed = key_pos[None, :] <= query_pos[:, None]
        highest = lax.optimization_barrier(jnp.max(jnp.where(allowed, scores, -jnp.inf), axis=1, keepdims=True))
        weight = jnp.where(allowed, jnp.exp(scores - highest), 0.0)
        weight_total = lax.optimization_barrier(jnp.sum(weight, axis=1, keepdims=True))
        mixed_rows = jnp.dot(weight.astype(jnp.bfloat16), value_head, preferred_element_type=jnp.float32)
        return (mixed_rows / weight_total).astype(jnp.bfloat16)
    blocks_out = lax.map(one_block, jnp.arange(TOKEN_TOTAL // block_size, dtype=jnp.int32))
    return blocks_out.reshape(TOKEN_TOTAL, HDIM)

def block_targets(block_routes):
    flat_routes = block_routes.reshape(-1)
    onehot = (flat_routes[:, None] == jnp.arange(EXPERTS, dtype=jnp.int32)[None, :]).astype(jnp.int32)
    before = jnp.cumsum(onehot, axis=0) - onehot
    return flat_routes * CAP + lax.optimization_barrier(jnp.sum(before * onehot, axis=1))

def reference(queries, key_vectors, value_vectors, log_gate_sums, residual, out_weight, norm_gain, routes, route_weight, expert_gate, expert_up, expert_down, shared_gate, shared_up, shared_down):

    def by_head(matrix):
        return matrix.reshape(TOKEN_TOTAL, HEAD_TOTAL, HDIM).transpose(1, 0, 2)
    attended = lax.map(one_head, (by_head(queries), by_head(key_vectors), by_head(value_vectors), log_gate_sums.T))
    attended = attended.transpose(1, 0, 2).reshape(TOKEN_TOTAL, HEAD_TOTAL * HDIM)
    projected = jnp.dot(attended, out_weight, preferred_element_type=jnp.float32)
    mid = (residual.astype(jnp.float32) + projected).astype(jnp.bfloat16)
    mid_wide = mid.astype(jnp.float32)
    inverse = lax.rsqrt(lax.optimization_barrier(jnp.mean(mid_wide * mid_wide, axis=1, keepdims=True)) + EPSILON)
    normed = (mid_wide * inverse * norm_gain.astype(jnp.float32)).astype(jnp.bfloat16)
    shared_mid = silu_gate(jnp.dot(normed, shared_gate, preferred_element_type=jnp.float32), jnp.dot(normed, shared_up, preferred_element_type=jnp.float32)).astype(jnp.bfloat16)
    shared_out = jnp.dot(shared_mid, shared_down, preferred_element_type=jnp.float32)
    targets = jax.vmap(block_targets)(routes.reshape(N_SP, TOK_DEV, TOPK))
    local_rows = jnp.arange(TOK_DEV * TOPK, dtype=jnp.int32) // TOPK

    def block_owners(target_row, block_number):
        table = jnp.full((EXPERTS * CAP,), TOKEN_TOTAL, jnp.int32)
        return table.at[target_row].set(block_number * TOK_DEV + local_rows)
    owners = jax.vmap(block_owners)(targets, jnp.arange(N_SP, dtype=jnp.int32))
    owners = owners.reshape(N_SP, EXPERTS, CAP).transpose(1, 0, 2).reshape(EXPERTS, N_SP * CAP)
    padded = jnp.concatenate([normed, jnp.zeros((1, D), jnp.bfloat16)], axis=0)

    def one_expert(inputs):
        gate_weight, up_weight, down_weight, owner_rows = inputs
        row_values = padded[owner_rows]
        hidden = silu_gate(jnp.dot(row_values, gate_weight, preferred_element_type=jnp.float32), jnp.dot(row_values, up_weight, preferred_element_type=jnp.float32)).astype(jnp.bfloat16)
        return jnp.dot(hidden, down_weight, preferred_element_type=jnp.float32).astype(jnp.bfloat16)
    produced = lax.map(one_expert, (expert_gate, expert_up, expert_down, owners))
    expert_ids = targets // CAP
    slot_rank = targets % CAP
    block_ids = jnp.arange(N_SP, dtype=jnp.int32)[:, None]
    flat_index = (expert_ids * (N_SP * CAP) + block_ids * CAP + slot_rank).reshape(-1)
    picked = produced.reshape(EXPERTS * N_SP * CAP, D)[flat_index].astype(jnp.float32).reshape(TOKEN_TOTAL, TOPK, D)
    routed = lax.optimization_barrier(jnp.sum(picked * route_weight[:, :, None], axis=1))
    return (mid_wide + shared_out + routed).astype(jnp.bfloat16)
```

```python
import functools
import math

import jax
import jax.numpy as jnp
from jax import lax
from jax.experimental import pallas as pl
from jax.experimental.pallas import tpu as pltpu
from jax.sharding import PartitionSpec as P

HDIM = 64


EPSILON = 1e-06


def silu_gate(gate_part, up_part):
    return jax.nn.silu(gate_part) * up_part


def slot_targets(routes, experts_all, capacity):
    flat_routes = routes.reshape(-1)
    onehot = (flat_routes[:, None] == jnp.arange(experts_all, dtype=jnp.int32)[None, :]).astype(
        jnp.int32
    )
    before = jnp.cumsum(onehot, axis=0) - onehot
    return flat_routes * capacity + jnp.sum(before * onehot, axis=1)


def keep_state(fold_state):
    return fold_state


def shards(
    queries,
    key_vectors,
    value_vectors,
    log_gate_sums,
    residual,
    out_weight,
    norm_gain,
    routes,
    route_weight,
    expert_gate,
    expert_up,
    expert_down,
    shared_gate,
    shared_up,
    shared_down,
):
    tok_dev = queries.shape[0]
    head_dim = HDIM
    local_heads = log_gate_sums.shape[1]
    local_width = residual.shape[1]
    model_width = norm_gain.shape[0]
    score_scale = head_dim ** (-0.5)
    seq_first = lax.axis_index("sp") * tok_dev
    query_heads = queries.reshape(tok_dev, local_heads, head_dim)
    query_pos = seq_first + jnp.arange(tok_dev, dtype=jnp.int32)
    own_gates = log_gate_sums.T
    all_gates = lax.all_gather(log_gate_sums, "sp", axis=0, tiled=True)
    initial = (
        jnp.full((local_heads, tok_dev), -1e30, jnp.float32),
        jnp.zeros((local_heads, tok_dev), jnp.float32),
        jnp.zeros((local_heads, tok_dev, head_dim), jnp.float32),
    )
    key_heads = key_vectors.reshape(tok_dev, local_heads, head_dim)
    value_heads = value_vectors.reshape(tok_dev, local_heads, head_dim)
    key_part = lax.all_gather(key_heads, "sp", axis=0, tiled=True)
    value_part = lax.all_gather(value_heads, "sp", axis=0, tiled=True)
    part_rows = key_part.shape[0]
    block_size = math.gcd(part_rows, 512)
    key_blocks = key_part.reshape(part_rows // block_size, block_size, local_heads, head_dim)
    value_blocks = value_part.reshape(part_rows // block_size, block_size, local_heads, head_dim)

    def one_block(fold_state, inputs):
        key_block, value_block, block_number = inputs
        block_first = block_number * block_size

        def compute(old_state):
            running_max, weight_total, summed = old_state
            gate_block = lax.dynamic_slice_in_dim(all_gates, block_first, block_size, 0).T
            scores = (
                jnp.einsum(
                    "qhd,khd->hqk", query_heads, key_block, preferred_element_type=jnp.float32
                )
                * score_scale
            )
            scores = scores + own_gates[:, :, None] - gate_block[:, None, :]
            key_pos = block_first + jnp.arange(block_size, dtype=jnp.int32)
            allowed = (key_pos[None, :] <= query_pos[:, None])[None]
            newmax = jnp.maximum(running_max, jnp.max(jnp.where(allowed, scores, -jnp.inf), axis=2))
            factor = jnp.exp(running_max - newmax)
            weight = jnp.where(allowed, jnp.exp(scores - newmax[:, :, None]), 0.0)
            weight_total = weight_total * factor + jnp.sum(weight, axis=2)
            summed = summed * factor[:, :, None] + jnp.einsum(
                "hqk,khd->hqd",
                weight.astype(jnp.bfloat16),
                value_block,
                preferred_element_type=jnp.float32,
            )
            return (newmax, weight_total, summed)

        useful = block_first <= seq_first + tok_dev - 1
        return (lax.cond(useful, compute, keep_state, fold_state), None)

    numbers = jnp.arange(part_rows // block_size, dtype=jnp.int32)
    result_state, _ = lax.scan(one_block, initial, (key_blocks, value_blocks, numbers))
    running_max, weight_total, summed = result_state
    attended = (summed / weight_total[:, :, None]).astype(jnp.bfloat16)
    attended = attended.transpose(1, 0, 2).reshape(tok_dev, local_heads * head_dim)
    weight_rows = out_weight
    projected = jnp.dot(
        lax.all_gather(attended, "tp", axis=1, tiled=True),
        weight_rows,
        preferred_element_type=jnp.float32,
    )
    mid = (residual.astype(jnp.float32) + projected).astype(jnp.bfloat16)
    mid_wide = mid.astype(jnp.float32)
    feature_first = lax.axis_index("tp") * local_width
    squares = lax.psum(jnp.sum(mid_wide * mid_wide, axis=1), "tp")
    inverse = lax.rsqrt(squares / model_width + EPSILON)
    own_gain = lax.dynamic_slice_in_dim(norm_gain, feature_first, local_width, 0).astype(
        jnp.float32
    )
    normed_own = (mid_wide * inverse[:, None] * own_gain[None, :]).astype(jnp.bfloat16)
    normed = lax.all_gather(normed_own, "tp", axis=1, tiled=True)
    shared_mid = silu_gate(
        jnp.dot(normed, shared_gate, preferred_element_type=jnp.float32),
        jnp.dot(normed, shared_up, preferred_element_type=jnp.float32),
    ).astype(jnp.bfloat16)
    weight_rows = shared_down
    shared_out = jnp.dot(
        lax.all_gather(shared_mid, "tp", axis=1, tiled=True),
        weight_rows,
        preferred_element_type=jnp.float32,
    )
    exp_dev = expert_gate.shape[0]
    sp_count = lax.axis_size("sp")
    experts_all = exp_dev * sp_count
    top_count = routes.shape[1]
    capacity = 5 * tok_dev * top_count // (4 * experts_all)
    targets = slot_targets(routes, experts_all, capacity)
    owners = (
        jnp.full((experts_all * capacity,), tok_dev, jnp.int32)
        .at[targets]
        .set(jnp.arange(tok_dev * top_count, dtype=jnp.int32) // top_count)
    )
    padded = jnp.concatenate(
        [normed_own, jnp.zeros((1, normed_own.shape[1]), jnp.bfloat16)], axis=0
    )
    outgoing = padded[owners].reshape(sp_count, exp_dev, capacity, normed_own.shape[1])
    rows_all = lax.all_gather(
        lax.all_to_all(outgoing, "sp", split_axis=0, concat_axis=0, tiled=True),
        "tp",
        axis=3,
        tiled=True,
    )
    gate_part = jnp.einsum(
        "secd,edf->secf", rows_all, expert_gate, preferred_element_type=jnp.float32
    )
    up_part = jnp.einsum("secd,edf->secf", rows_all, expert_up, preferred_element_type=jnp.float32)
    hidden = silu_gate(gate_part, up_part).astype(jnp.bfloat16)
    hidden_all = lax.all_gather(hidden, "tp", axis=3, tiled=True)
    produced = jnp.einsum(
        "secf,efd->secd", hidden_all, expert_down, preferred_element_type=jnp.float32
    ).astype(jnp.bfloat16)
    returned = lax.all_to_all(produced, "sp", split_axis=0, concat_axis=0, tiled=True)
    returned_flat = returned.reshape(experts_all * capacity, local_width)
    picked = returned_flat[targets].astype(jnp.float32).reshape(tok_dev, top_count, local_width)
    routed = jnp.sum(picked * route_weight[:, :, None], axis=1)
    return (mid_wide + shared_out + routed).astype(jnp.bfloat16)


def peer(sp=None, tp=None):
    named = {}
    if sp is not None:
        named["sp"] = sp
    if tp is not None:
        named["tp"] = tp
    return named


def send(src, dst, send_sem, recv_sem, to):
    return pltpu.make_async_remote_copy(
        src_ref=src,
        dst_ref=dst,
        send_sem=send_sem,
        recv_sem=recv_sem,
        device_id=to,
        device_id_type=pl.DeviceIdType.MESH,
    )


def greet(to):
    pl.semaphore_signal(
        pltpu.get_barrier_semaphore(), inc=1, device_id=to, device_id_type=pl.DeviceIdType.MESH
    )


def kv_kernel(
    n_sp,
    k_ref,
    v_ref,
    g_ref,
    gate_ref,
    up_ref,
    k_all,
    v_all,
    g_all,
    gate_all,
    up_all,
    up_send,
    up_recv,
    side_send,
    side_recv,
    w_send,
    w_recv,
    own_sem,
):
    me = lax.axis_index("sp")
    tp = lax.axis_index("tp")
    z, core = me // 2, me % 2
    depth = n_sp // 2
    partner = z * 2 + (1 - core)
    has_above = z + 1 < depth
    greet(peer(sp=partner))
    for d in range(1, 4):
        greet(peer(tp=(tp + d) % 4))

    @pl.when(has_above)
    def _():
        greet(peer(sp=(me + 2) % n_sp))

    @pl.when(z > 0)
    def _():
        greet(peer(sp=(me - 2 + n_sp) % n_sp))

    count = 4 + jnp.where(has_above, 1, 0) + jnp.where(z > 0, 1, 0)
    pl.semaphore_wait(pltpu.get_barrier_semaphore(), count)
    above = peer(sp=(me + 2) % n_sp)
    blocks = (k_ref, v_ref, g_ref)
    wholes = (k_all, v_all, g_all)

    def upward(s, i):
        slot = ((z - s + depth) % depth) * 2 + core
        src = blocks[i] if s == 0 else wholes[i].at[slot]
        return send(src, wholes[i].at[slot], up_send.at[s, i], up_recv.at[s, i], above)

    def arriving(s, i):
        slot = ((z - 1 - s + 2 * depth) % depth) * 2 + core
        return send(blocks[i], wholes[i].at[slot], up_send.at[s, i], up_recv.at[s, i], above)

    def sideways(s, i):
        slot = ((z - s + depth) % depth) * 2 + core
        src = blocks[i] if s == 0 else wholes[i].at[slot]
        return send(src, wholes[i].at[slot], side_send.at[s, i], side_recv.at[s, i], peer(sp=partner))

    def from_side(s, i):
        slot = ((z - s + depth) % depth) * 2 + (1 - core)
        return send(
            blocks[i], wholes[i].at[slot], side_send.at[s, i], side_recv.at[s, i], peer(sp=partner)
        )

    weights = ((gate_ref, gate_all), (up_ref, up_all))

    def weight_out(d, i):
        to = (tp + d) % 4
        return send(
            weights[i][0].at[to],
            weights[i][1].at[tp],
            w_send.at[d - 1, i],
            w_recv.at[d - 1, i],
            peer(tp=to),
        )

    def weight_in(d, i):
        source = (tp - d + 4) % 4
        return send(
            weights[i][0].at[source],
            weights[i][1].at[source],
            w_send.at[d - 1, i],
            w_recv.at[d - 1, i],
            peer(tp=source),
        )

    three = range(3)

    @pl.when(has_above)
    def _():
        for i in three:
            upward(0, i).start()

    for i in three:
        sideways(0, i).start()
    for d in (2, 1, 3):
        for i in range(2):
            weight_out(d, i).start()
    own = [pltpu.make_async_copy(blocks[i], wholes[i].at[me], own_sem.at[i]) for i in three]
    for copy in own:
        copy.start()
    for s in range(1, depth):

        @pl.when(z >= s)
        def _():
            for i in three:
                arriving(s - 1, i).wait_recv()
                if s < depth - 1:

                    @pl.when(has_above)
                    def _():
                        upward(s, i).start()

                sideways(s, i).start()

    for s in range(depth):

        @pl.when(z >= s)
        def _():
            for i in three:
                from_side(s, i).wait_recv()
                sideways(s, i).wait_send()
            if s < depth - 1:

                @pl.when(has_above)
                def _():
                    for i in three:
                        upward(s, i).wait_send()

    for copy in own:
        copy.wait()
    for d in range(1, 4):
        for i in range(2):
            weight_in(d, i).wait_recv()
            weight_out(d, i).wait_send()


def gather_kernel(block, whole, send_sem, recv_sem, own_sem):
    tp = lax.axis_index("tp")
    rows, width = block.shape
    half = rows // 2
    x_near = tp // 2 * 2 + (1 - tp % 2)
    y_near = (tp + 2) % 4
    nears = (x_near, y_near)
    for near in nears:
        greet(peer(tp=near))
    pl.semaphore_wait(pltpu.get_barrier_semaphore(), 2)

    def place(owner, part):
        return whole.at[pl.ds(part * half, half), pl.ds(pl.multiple_of(owner * width, width), width)]

    def outward(axis, part):
        return send(
            block.at[pl.ds(part * half, half)],
            place(tp, part),
            send_sem.at[axis, part],
            recv_sem.at[axis, part],
            peer(tp=nears[axis]),
        )

    def inward(axis, part):
        return send(
            block.at[pl.ds(part * half, half)],
            place(nears[axis], part),
            send_sem.at[axis, part],
            recv_sem.at[axis, part],
            peer(tp=nears[axis]),
        )

    far = (x_near + 2) % 4

    def relay(axis):
        return send(
            place(nears[1 - axis], axis),
            place(nears[1 - axis], axis),
            send_sem.at[axis, 2],
            recv_sem.at[axis, 2],
            peer(tp=nears[axis]),
        )

    def relayed(axis):
        return send(
            place(far, axis),
            place(far, axis),
            send_sem.at[axis, 2],
            recv_sem.at[axis, 2],
            peer(tp=nears[axis]),
        )

    for order in range(2):
        for axis in range(2):
            outward(axis, (1 - axis + order) % 2).start()
    own = pltpu.make_async_copy(
        block, whole.at[:, pl.ds(pl.multiple_of(tp * width, width), width)], own_sem
    )
    own.start()
    for axis in range(2):
        inward(1 - axis, axis).wait_recv()
        relay(axis).start()
    for axis in range(2):
        inward(axis, 1 - (1 - axis)).wait_recv()
        relayed(axis).wait_recv()
        relay(axis).wait_send()
        for part in range(2):
            outward(axis, part).wait_send()
    own.wait()


def any_space(count):
    return [pl.BlockSpec(memory_space=pl.ANY)] * count


def vmem_space(count):
    return [pl.BlockSpec(memory_space=pltpu.VMEM)] * count


def gather_features(block, number):
    rows, width = block.shape
    return pl.pallas_call(
        gather_kernel,
        name=f"gather_{number}",
        out_shape=jax.ShapeDtypeStruct((rows, 4 * width), block.dtype),
        in_specs=vmem_space(1),
        out_specs=pl.BlockSpec(memory_space=pl.ANY),
        scratch_shapes=[
            pltpu.SemaphoreType.DMA((2, 3)),
            pltpu.SemaphoreType.DMA((2, 3)),
            pltpu.SemaphoreType.DMA,
        ],
        compiler_params=pltpu.CompilerParams(collective_id=number, has_side_effects=True),
    )(block)


def dispatch_kernel(
    n_sp, rows, mid, down, rows_all, mid_all, down_all, z_send, z_recv, t_send, t_recv, own_sem
):
    me = lax.axis_index("sp")
    tp = lax.axis_index("tp")
    width = mid.shape[1]
    for d in range(1, n_sp):
        greet(peer(sp=(me + d) % n_sp))
    for d in range(1, 4):
        greet(peer(tp=(tp + d) % 4))
    pl.semaphore_wait(pltpu.get_barrier_semaphore(), n_sp - 1 + 3)

    def columns(owner):
        return mid_all.at[:, pl.ds(pl.multiple_of(owner * width, width), width)]

    def row_copy(d):
        to = (me + d) % n_sp
        return send(rows.at[to], rows_all.at[me], z_send.at[d], z_recv.at[d], peer(sp=to))

    def row_arrival(d):
        source = (me - d + n_sp) % n_sp
        return send(rows.at[source], rows_all.at[source], z_send.at[d], z_recv.at[d], peer(sp=source))

    def side_copies(d):
        to = (tp + d) % 4
        return (
            send(mid, columns(tp), t_send.at[d, 0], t_recv.at[d, 0], peer(tp=to)),
            send(down.at[to], down_all.at[tp], t_send.at[d, 1], t_recv.at[d, 1], peer(tp=to)),
        )

    def side_arrivals(d):
        source = (tp - d + 4) % 4
        return (
            send(mid, columns(source), t_send.at[d, 0], t_recv.at[d, 0], peer(tp=source)),
            send(down.at[source], down_all.at[source], t_send.at[d, 1], t_recv.at[d, 1], peer(tp=source)),
        )

    half = n_sp // 2
    for d in sorted(range(1, n_sp), key=lambda d: abs(d - half)):
        row_copy(d).start()
    for d in (2, 1, 3):
        for copy in side_copies(d):
            copy.start()
    own = (
        pltpu.make_async_copy(rows.at[me], rows_all.at[me], own_sem.at[0]),
        pltpu.make_async_copy(mid, columns(tp), own_sem.at[1]),
    )
    for copy in own:
        copy.start()
    for d in range(1, n_sp):
        row_arrival(d).wait_recv()
        row_copy(d).wait_send()
    for d in range(1, 4):
        for copy in side_arrivals(d):
            copy.wait_recv()
        for copy in side_copies(d):
            copy.wait_send()
    for copy in own:
        copy.wait()


def return_kernel(n_sp, produced, final, stage, t_send, t_recv, z_send, z_recv, own_sem):
    me = lax.axis_index("sp")
    tp = lax.axis_index("tp")
    for d in range(1, n_sp):
        greet(peer(sp=(me + d) % n_sp))
    for d in range(1, 4):
        greet(peer(tp=(tp + d) % 4))
    pl.semaphore_wait(pltpu.get_barrier_semaphore(), n_sp - 1 + 3)

    def target(d):
        return (me + d) % n_sp

    def landing(d, owner):
        return final.at[me, owner] if d == 0 else stage.at[target(d), owner]

    def side_copy(d, r):
        to = (tp + r) % 4
        return send(
            produced.at[to, target(d)], landing(d, tp), t_send.at[d, r], t_recv.at[d, r], peer(tp=to)
        )

    def side_arrival(d, r):
        source = (tp - r + 4) % 4
        return send(
            produced.at[source, target(d)],
            landing(d, source),
            t_send.at[d, r],
            t_recv.at[d, r],
            peer(tp=source),
        )

    def back_copy(d, r):
        owner = (tp - r + 4) % 4
        src = produced.at[tp, target(d)] if r == 0 else stage.at[target(d), owner]
        return send(
            src, final.at[me, owner], z_send.at[d, r], z_recv.at[d, r], peer(sp=target(d))
        )

    def back_arrival(d, r):
        owner = (tp - r + 4) % 4
        source = (me - d + n_sp) % n_sp
        return send(
            produced.at[tp, source],
            final.at[source, owner],
            z_send.at[d, r],
            z_recv.at[d, r],
            peer(sp=source),
        )

    half = n_sp // 2
    order = sorted(range(1, n_sp), key=lambda d: abs(d - half))
    for d in order:
        back_copy(d, 0).start()
    for d in order + [0]:
        for r in (2, 1, 3):
            side_copy(d, r).start()
    own = pltpu.make_async_copy(produced.at[tp, me], final.at[me, tp], own_sem)
    own.start()
    for d in order:
        for r in (1, 3, 2):
            side_arrival(d, r).wait_recv()
            back_copy(d, r).start()
    for r in range(1, 4):
        side_arrival(0, r).wait_recv()
    for d in range(n_sp):
        for r in range(1, 4):
            side_copy(d, r).wait_send()
    for d in order:
        for r in range(4):
            back_arrival(d, r).wait_recv()
            back_copy(d, r).wait_send()
    own.wait()


def attention_kernel(q_ref, k_ref, v_ref, g_ref, o_ref, top, total, summed):
    me = lax.axis_index("sp")
    heads = g_ref.shape[1]
    rows = q_ref.shape[0]
    dim = q_ref.shape[1] // heads
    for h in range(heads):
        top[h] = jnp.full(top.shape[1:], -1e30, jnp.float32)
        total[h] = jnp.zeros(total.shape[1:], jnp.float32)
        summed[h] = jnp.zeros(summed.shape[1:], jnp.float32)

    def fold(j, masked):
        for h in range(heads):
            columns = slice(h * dim, (h + 1) * dim)
            scores = lax.dot_general(
                q_ref[:, columns],
                k_ref[j, :, columns],
                (((1,), (1,)), ((), ())),
                preferred_element_type=jnp.float32,
            )
            scores = scores - g_ref[j, h : h + 1, :]
            if masked:
                row = lax.broadcasted_iota(jnp.int32, scores.shape, 0)
                column = lax.broadcasted_iota(jnp.int32, scores.shape, 1)
                scores = jnp.where(column <= row, scores, -jnp.inf)
            old = top[h]
            new = jnp.maximum(old, jnp.max(scores, axis=1, keepdims=True))
            factor = jnp.exp(old - new)
            weight = jnp.exp(scores - new)
            total[h] = total[h] * factor + jnp.sum(weight, axis=1, keepdims=True)
            summed[h] = summed[h] * factor + jnp.dot(
                weight.astype(jnp.bfloat16), v_ref[j, :, columns], preferred_element_type=jnp.float32
            )
            top[h] = new

    def one(j, carry):
        fold(j, False)
        return carry

    lax.fori_loop(0, me, one, 0)
    fold(me, True)
    for h in range(heads):
        o_ref[:, h * dim : (h + 1) * dim] = (summed[h] / total[h]).astype(o_ref.dtype)


def fast_shards(
    queries,
    key_vectors,
    value_vectors,
    log_gate_sums,
    residual,
    out_weight,
    norm_gain,
    routes,
    route_weight,
    expert_gate,
    expert_up,
    expert_down,
    shared_gate,
    shared_up,
    shared_down,
):
    n_sp = lax.axis_size("sp")
    tp = lax.axis_index("tp")
    tok_dev = queries.shape[0]
    heads = log_gate_sums.shape[1]
    local_width = residual.shape[1]
    model_width = norm_gain.shape[0]
    exp_dev = expert_gate.shape[0]
    experts_all = exp_dev * n_sp
    top_count = routes.shape[1]
    capacity = 5 * tok_dev * top_count // (4 * experts_all)
    depth = n_sp // 2

    def like(shape, array):
        return jax.ShapeDtypeStruct(shape, array.dtype)

    gates = log_gate_sums.T
    k_all, v_all, g_all, gate_all, up_all = pl.pallas_call(
        functools.partial(kv_kernel, n_sp),
        name="kv_share",
        out_shape=(
            like((n_sp,) + key_vectors.shape, key_vectors),
            like((n_sp,) + value_vectors.shape, value_vectors),
            like((n_sp,) + gates.shape, gates),
            like(expert_gate.shape, expert_gate),
            like(expert_up.shape, expert_up),
        ),
        in_specs=vmem_space(3) + any_space(2),
        out_specs=tuple(any_space(5)),
        scratch_shapes=[
            pltpu.SemaphoreType.DMA((depth, 3)),
            pltpu.SemaphoreType.DMA((depth, 3)),
            pltpu.SemaphoreType.DMA((depth, 3)),
            pltpu.SemaphoreType.DMA((depth, 3)),
            pltpu.SemaphoreType.DMA((3, 2)),
            pltpu.SemaphoreType.DMA((3, 2)),
            pltpu.SemaphoreType.DMA((3,)),
        ],
        compiler_params=pltpu.CompilerParams(collective_id=1, has_side_effects=True),
    )(key_vectors, value_vectors, gates, expert_gate, expert_up)

    scaled = (queries.astype(jnp.float32) * HDIM ** (-0.5)).astype(jnp.bfloat16)
    attended = pl.pallas_call(
        attention_kernel,
        name="attention",
        out_shape=like(queries.shape, queries),
        in_specs=vmem_space(4),
        out_specs=pl.BlockSpec(memory_space=pltpu.VMEM),
        scratch_shapes=[
            pltpu.VMEM((heads, tok_dev, 1), jnp.float32),
            pltpu.VMEM((heads, tok_dev, 1), jnp.float32),
            pltpu.VMEM((heads, tok_dev, HDIM), jnp.float32),
        ],
        compiler_params=pltpu.CompilerParams(vmem_limit_bytes=40 * 1024 * 1024),
    )(scaled, k_all, v_all, g_all)

    flat_routes = routes.reshape(-1)
    onehot = flat_routes[:, None] == jnp.arange(experts_all, dtype=jnp.int32)[None, :]
    pairs = tok_dev * top_count
    earlier = (
        jnp.arange(pairs, dtype=jnp.int32)[None, :] < jnp.arange(pairs, dtype=jnp.int32)[:, None]
    ).astype(jnp.bfloat16)
    before = jnp.dot(earlier, onehot.astype(jnp.bfloat16), preferred_element_type=jnp.float32)
    rank = jnp.sum(jnp.where(onehot, before, 0.0), axis=1).astype(jnp.int32)
    rank = rank.reshape(tok_dev, top_count)
    targets = routes * capacity + rank
    here = jnp.where(routes % exp_dev == tp, routes // exp_dev * capacity + rank, -1)
    slots = jnp.arange(n_sp * capacity, dtype=jnp.int32)[:, None]
    chosen = slots == here[:, 0][None, :]
    for k in range(1, top_count):
        chosen = chosen | (slots == here[:, k][None, :])
    chosen = chosen.astype(jnp.bfloat16)

    attended_all = gather_features(attended, 2)
    projected = jnp.dot(attended_all, out_weight, preferred_element_type=jnp.float32)
    mid = (residual.astype(jnp.float32) + projected).astype(jnp.bfloat16)
    mid_all = gather_features(mid, 3).astype(jnp.float32)
    inverse = lax.rsqrt(jnp.mean(mid_all * mid_all, axis=1, keepdims=True) + EPSILON)
    normed = (mid_all * inverse * norm_gain.astype(jnp.float32)[None, :]).astype(jnp.bfloat16)
    rows = jnp.dot(chosen, normed, preferred_element_type=jnp.float32).astype(jnp.bfloat16)
    rows = rows.reshape(n_sp, capacity, model_width)
    shared_mid = silu_gate(
        jnp.dot(normed, shared_gate, preferred_element_type=jnp.float32),
        jnp.dot(normed, shared_up, preferred_element_type=jnp.float32),
    ).astype(jnp.bfloat16)

    rows_all, shared_all, down_all = pl.pallas_call(
        functools.partial(dispatch_kernel, n_sp),
        name="dispatch",
        out_shape=(
            like(rows.shape, rows),
            like((tok_dev, 4 * shared_mid.shape[1]), shared_mid),
            like(expert_down.shape, expert_down),
        ),
        in_specs=vmem_space(2) + any_space(1),
        out_specs=tuple(any_space(3)),
        scratch_shapes=[
            pltpu.SemaphoreType.DMA((n_sp,)),
            pltpu.SemaphoreType.DMA((n_sp,)),
            pltpu.SemaphoreType.DMA((4, 2)),
            pltpu.SemaphoreType.DMA((4, 2)),
            pltpu.SemaphoreType.DMA((2,)),
        ],
        compiler_params=pltpu.CompilerParams(collective_id=4, has_side_effects=True),
    )(rows, shared_mid, expert_down)

    def with_own(whole, shard):
        block = lax.dynamic_slice_in_dim(shard, tp, 1, 0)
        return lax.dynamic_update_slice_in_dim(whole, block, tp, 0)

    gate_all = with_own(gate_all, expert_gate)
    up_all = with_own(up_all, expert_up)
    down_all = with_own(down_all, expert_down)
    flat_rows = rows_all.reshape(n_sp * capacity, model_width)
    hidden = jnp.concatenate(
        [
            silu_gate(
                jnp.dot(flat_rows, gate_all[t], preferred_element_type=jnp.float32),
                jnp.dot(flat_rows, up_all[t], preferred_element_type=jnp.float32),
            ).astype(jnp.bfloat16)
            for t in range(4)
        ],
        axis=1,
    )
    produced = jnp.stack(
        [
            jnp.dot(hidden, down_all[t], preferred_element_type=jnp.float32).astype(jnp.bfloat16)
            for t in range(4)
        ]
    ).reshape(4, n_sp, capacity, local_width)

    final = pl.pallas_call(
        functools.partial(return_kernel, n_sp),
        name="give_back",
        out_shape=like((n_sp, 4, capacity, local_width), produced),
        in_specs=vmem_space(1),
        out_specs=pl.BlockSpec(memory_space=pl.ANY),
        scratch_shapes=[
            pltpu.VMEM((n_sp, 4, capacity, local_width), jnp.bfloat16),
            pltpu.SemaphoreType.DMA((n_sp, 4)),
            pltpu.SemaphoreType.DMA((n_sp, 4)),
            pltpu.SemaphoreType.DMA((n_sp, 4)),
            pltpu.SemaphoreType.DMA((n_sp, 4)),
            pltpu.SemaphoreType.DMA,
        ],
        compiler_params=pltpu.CompilerParams(collective_id=5, has_side_effects=True),
    )(produced)

    shared_out = jnp.dot(shared_all, shared_down, preferred_element_type=jnp.float32)
    returned = final.reshape(experts_all * capacity, local_width)
    places = jnp.arange(experts_all * capacity, dtype=jnp.int32)[None, :]
    result = mid.astype(jnp.float32) + shared_out
    for k in range(top_count):
        pick = (places == targets[:, k][:, None]).astype(jnp.bfloat16)
        picked = jnp.dot(pick, returned, preferred_element_type=jnp.float32)
        result = result + picked * route_weight[:, k][:, None]
    return result.astype(jnp.bfloat16)


def solution(mesh):
    placed = (
        P("sp", "tp"),
        P("sp", "tp"),
        P("sp", "tp"),
        P("sp", "tp"),
        P("sp", "tp"),
        P(None, "tp"),
        P(),
        P("sp", None),
        P("sp", None),
        P("sp", None, "tp"),
        P("sp", None, "tp"),
        P("sp", None, "tp"),
        P(None, "tp"),
        P(None, "tp"),
        P(None, "tp"),
    )
    fits = mesh.shape["tp"] == 4 and mesh.shape["sp"] % 2 == 0 and mesh.shape["sp"] <= 16
    return jax.shard_map(
        fast_shards if fits else shards, mesh=mesh, in_specs=placed, out_specs=P("sp", "tp"), check_vma=False
    )
```

```python
import functools
import math

import jax
import jax.numpy as jnp
from jax import lax
from jax.experimental import pallas as pl
from jax.experimental.pallas import tpu as pltpu
from jax.sharding import PartitionSpec as P

HDIM = 64


EPSILON = 1e-06


def silu_gate(gate_part, up_part):
    return jax.nn.silu(gate_part) * up_part


def slot_targets(routes, experts_all, capacity):
    flat_routes = routes.reshape(-1)
    onehot = (flat_routes[:, None] == jnp.arange(experts_all, dtype=jnp.int32)[None, :]).astype(
        jnp.int32
    )
    before = jnp.cumsum(onehot, axis=0) - onehot
    return flat_routes * capacity + jnp.sum(before * onehot, axis=1)


def keep_state(fold_state):
    return fold_state


def shards(
    queries,
    key_vectors,
    value_vectors,
    log_gate_sums,
    residual,
    out_weight,
    norm_gain,
    routes,
    route_weight,
    expert_gate,
    expert_up,
    expert_down,
    shared_gate,
    shared_up,
    shared_down,
):
    tok_dev = queries.shape[0]
    head_dim = HDIM
    local_heads = log_gate_sums.shape[1]
    local_width = residual.shape[1]
    model_width = norm_gain.shape[0]
    score_scale = head_dim ** (-0.5)
    seq_first = lax.axis_index("sp") * tok_dev
    query_heads = queries.reshape(tok_dev, local_heads, head_dim)
    query_pos = seq_first + jnp.arange(tok_dev, dtype=jnp.int32)
    own_gates = log_gate_sums.T
    all_gates = lax.all_gather(log_gate_sums, "sp", axis=0, tiled=True)
    initial = (
        jnp.full((local_heads, tok_dev), -1e30, jnp.float32),
        jnp.zeros((local_heads, tok_dev), jnp.float32),
        jnp.zeros((local_heads, tok_dev, head_dim), jnp.float32),
    )
    key_heads = key_vectors.reshape(tok_dev, local_heads, head_dim)
    value_heads = value_vectors.reshape(tok_dev, local_heads, head_dim)
    key_part = lax.all_gather(key_heads, "sp", axis=0, tiled=True)
    value_part = lax.all_gather(value_heads, "sp", axis=0, tiled=True)
    part_rows = key_part.shape[0]
    block_size = math.gcd(part_rows, 512)
    key_blocks = key_part.reshape(part_rows // block_size, block_size, local_heads, head_dim)
    value_blocks = value_part.reshape(part_rows // block_size, block_size, local_heads, head_dim)

    def one_block(fold_state, inputs):
        key_block, value_block, block_number = inputs
        block_first = block_number * block_size

        def compute(old_state):
            running_max, weight_total, summed = old_state
            gate_block = lax.dynamic_slice_in_dim(all_gates, block_first, block_size, 0).T
            scores = (
                jnp.einsum(
                    "qhd,khd->hqk", query_heads, key_block, preferred_element_type=jnp.float32
                )
                * score_scale
            )
            scores = scores + own_gates[:, :, None] - gate_block[:, None, :]
            key_pos = block_first + jnp.arange(block_size, dtype=jnp.int32)
            allowed = (key_pos[None, :] <= query_pos[:, None])[None]
            newmax = jnp.maximum(running_max, jnp.max(jnp.where(allowed, scores, -jnp.inf), axis=2))
            factor = jnp.exp(running_max - newmax)
            weight = jnp.where(allowed, jnp.exp(scores - newmax[:, :, None]), 0.0)
            weight_total = weight_total * factor + jnp.sum(weight, axis=2)
            summed = summed * factor[:, :, None] + jnp.einsum(
                "hqk,khd->hqd",
                weight.astype(jnp.bfloat16),
                value_block,
                preferred_element_type=jnp.float32,
            )
            return (newmax, weight_total, summed)

        useful = block_first <= seq_first + tok_dev - 1
        return (lax.cond(useful, compute, keep_state, fold_state), None)

    numbers = jnp.arange(part_rows // block_size, dtype=jnp.int32)
    result_state, _ = lax.scan(one_block, initial, (key_blocks, value_blocks, numbers))
    running_max, weight_total, summed = result_state
    attended = (summed / weight_total[:, :, None]).astype(jnp.bfloat16)
    attended = attended.transpose(1, 0, 2).reshape(tok_dev, local_heads * head_dim)
    weight_rows = out_weight
    projected = jnp.dot(
        lax.all_gather(attended, "tp", axis=1, tiled=True),
        weight_rows,
        preferred_element_type=jnp.float32,
    )
    mid = (residual.astype(jnp.float32) + projected).astype(jnp.bfloat16)
    mid_wide = mid.astype(jnp.float32)
    feature_first = lax.axis_index("tp") * local_width
    squares = lax.psum(jnp.sum(mid_wide * mid_wide, axis=1), "tp")
    inverse = lax.rsqrt(squares / model_width + EPSILON)
    own_gain = lax.dynamic_slice_in_dim(norm_gain, feature_first, local_width, 0).astype(
        jnp.float32
    )
    normed_own = (mid_wide * inverse[:, None] * own_gain[None, :]).astype(jnp.bfloat16)
    normed = lax.all_gather(normed_own, "tp", axis=1, tiled=True)
    shared_mid = silu_gate(
        jnp.dot(normed, shared_gate, preferred_element_type=jnp.float32),
        jnp.dot(normed, shared_up, preferred_element_type=jnp.float32),
    ).astype(jnp.bfloat16)
    weight_rows = shared_down
    shared_out = jnp.dot(
        lax.all_gather(shared_mid, "tp", axis=1, tiled=True),
        weight_rows,
        preferred_element_type=jnp.float32,
    )
    exp_dev = expert_gate.shape[0]
    sp_count = lax.axis_size("sp")
    experts_all = exp_dev * sp_count
    top_count = routes.shape[1]
    capacity = 5 * tok_dev * top_count // (4 * experts_all)
    targets = slot_targets(routes, experts_all, capacity)
    owners = (
        jnp.full((experts_all * capacity,), tok_dev, jnp.int32)
        .at[targets]
        .set(jnp.arange(tok_dev * top_count, dtype=jnp.int32) // top_count)
    )
    padded = jnp.concatenate(
        [normed_own, jnp.zeros((1, normed_own.shape[1]), jnp.bfloat16)], axis=0
    )
    outgoing = padded[owners].reshape(sp_count, exp_dev, capacity, normed_own.shape[1])
    rows_all = lax.all_gather(
        lax.all_to_all(outgoing, "sp", split_axis=0, concat_axis=0, tiled=True),
        "tp",
        axis=3,
        tiled=True,
    )
    gate_part = jnp.einsum(
        "secd,edf->secf", rows_all, expert_gate, preferred_element_type=jnp.float32
    )
    up_part = jnp.einsum("secd,edf->secf", rows_all, expert_up, preferred_element_type=jnp.float32)
    hidden = silu_gate(gate_part, up_part).astype(jnp.bfloat16)
    hidden_all = lax.all_gather(hidden, "tp", axis=3, tiled=True)
    produced = jnp.einsum(
        "secf,efd->secd", hidden_all, expert_down, preferred_element_type=jnp.float32
    ).astype(jnp.bfloat16)
    returned = lax.all_to_all(produced, "sp", split_axis=0, concat_axis=0, tiled=True)
    returned_flat = returned.reshape(experts_all * capacity, local_width)
    picked = returned_flat[targets].astype(jnp.float32).reshape(tok_dev, top_count, local_width)
    routed = jnp.sum(picked * route_weight[:, :, None], axis=1)
    return (mid_wide + shared_out + routed).astype(jnp.bfloat16)


def peer(sp=None, tp=None):
    named = {}
    if sp is not None:
        named["sp"] = sp
    if tp is not None:
        named["tp"] = tp
    return named


def send(src, dst, send_sem, recv_sem, to):
    return pltpu.make_async_remote_copy(
        src_ref=src,
        dst_ref=dst,
        send_sem=send_sem,
        recv_sem=recv_sem,
        device_id=to,
        device_id_type=pl.DeviceIdType.MESH,
    )


def greet(to):
    pl.semaphore_signal(
        pltpu.get_barrier_semaphore(), inc=1, device_id=to, device_id_type=pl.DeviceIdType.MESH
    )


def kv_kernel(
    n_sp,
    k_ref,
    v_ref,
    g_ref,
    gate_ref,
    up_ref,
    k_all,
    v_all,
    g_all,
    gate_all,
    up_all,
    up_send,
    up_recv,
    side_send,
    side_recv,
    w_send,
    w_recv,
    own_sem,
):
    me = lax.axis_index("sp")
    tp = lax.axis_index("tp")
    z, core = me // 2, me % 2
    depth = n_sp // 2
    partner = z * 2 + (1 - core)
    has_above = z + 1 < depth
    greet(peer(sp=partner))
    for d in range(1, 4):
        greet(peer(tp=(tp + d) % 4))

    @pl.when(has_above)
    def _():
        greet(peer(sp=(me + 2) % n_sp))

    @pl.when(z > 0)
    def _():
        greet(peer(sp=(me - 2 + n_sp) % n_sp))

    count = 4 + jnp.where(has_above, 1, 0) + jnp.where(z > 0, 1, 0)
    pl.semaphore_wait(pltpu.get_barrier_semaphore(), count)
    above = peer(sp=(me + 2) % n_sp)
    blocks = (k_ref, v_ref, g_ref)
    wholes = (k_all, v_all, g_all)

    def upward(s, i):
        slot = ((z - s + depth) % depth) * 2 + core
        src = blocks[i] if s == 0 else wholes[i].at[slot]
        return send(src, wholes[i].at[slot], up_send.at[s, i], up_recv.at[s, i], above)

    def arriving(s, i):
        slot = ((z - 1 - s + 2 * depth) % depth) * 2 + core
        return send(blocks[i], wholes[i].at[slot], up_send.at[s, i], up_recv.at[s, i], above)

    def sideways(s, i):
        slot = ((z - s + depth) % depth) * 2 + core
        src = blocks[i] if s == 0 else wholes[i].at[slot]
        return send(src, wholes[i].at[slot], side_send.at[s, i], side_recv.at[s, i], peer(sp=partner))

    def from_side(s, i):
        slot = ((z - s + depth) % depth) * 2 + (1 - core)
        return send(
            blocks[i], wholes[i].at[slot], side_send.at[s, i], side_recv.at[s, i], peer(sp=partner)
        )

    weights = ((gate_ref, gate_all), (up_ref, up_all))

    def weight_out(d, i):
        to = (tp + d) % 4
        return send(
            weights[i][0].at[to],
            weights[i][1].at[tp],
            w_send.at[d - 1, i],
            w_recv.at[d - 1, i],
            peer(tp=to),
        )

    def weight_in(d, i):
        source = (tp - d + 4) % 4
        return send(
            weights[i][0].at[source],
            weights[i][1].at[source],
            w_send.at[d - 1, i],
            w_recv.at[d - 1, i],
            peer(tp=source),
        )

    three = range(3)

    @pl.when(has_above)
    def _():
        for i in three:
            upward(0, i).start()

    for i in three:
        sideways(0, i).start()
    for d in (2, 1, 3):
        for i in range(2):
            weight_out(d, i).start()
    own = [pltpu.make_async_copy(blocks[i], wholes[i].at[me], own_sem.at[i]) for i in three]
    for copy in own:
        copy.start()
    for s in range(1, depth):

        @pl.when(z >= s)
        def _():
            for i in three:
                arriving(s - 1, i).wait_recv()
                if s < depth - 1:

                    @pl.when(has_above)
                    def _():
                        upward(s, i).start()

                sideways(s, i).start()

    for s in range(depth):

        @pl.when(z >= s)
        def _():
            for i in three:
                from_side(s, i).wait_recv()
                sideways(s, i).wait_send()
            if s < depth - 1:

                @pl.when(has_above)
                def _():
                    for i in three:
                        upward(s, i).wait_send()

    for copy in own:
        copy.wait()
    for d in range(1, 4):
        for i in range(2):
            weight_in(d, i).wait_recv()
            weight_out(d, i).wait_send()


def gather_kernel(block, whole, send_sem, recv_sem, own_sem):
    tp = lax.axis_index("tp")
    rows, width = block.shape
    half = rows // 2
    x_near = tp // 2 * 2 + (1 - tp % 2)
    y_near = (tp + 2) % 4
    nears = (x_near, y_near)
    for near in nears:
        greet(peer(tp=near))
    pl.semaphore_wait(pltpu.get_barrier_semaphore(), 2)

    def place(owner, part):
        return whole.at[pl.ds(part * half, half), pl.ds(pl.multiple_of(owner * width, width), width)]

    def outward(axis, part):
        return send(
            block.at[pl.ds(part * half, half)],
            place(tp, part),
            send_sem.at[axis, part],
            recv_sem.at[axis, part],
            peer(tp=nears[axis]),
        )

    def inward(axis, part):
        return send(
            block.at[pl.ds(part * half, half)],
            place(nears[axis], part),
            send_sem.at[axis, part],
            recv_sem.at[axis, part],
            peer(tp=nears[axis]),
        )

    far = (x_near + 2) % 4

    def relay(axis):
        return send(
            place(nears[1 - axis], axis),
            place(nears[1 - axis], axis),
            send_sem.at[axis, 2],
            recv_sem.at[axis, 2],
            peer(tp=nears[axis]),
        )

    def relayed(axis):
        return send(
            place(far, axis),
            place(far, axis),
            send_sem.at[axis, 2],
            recv_sem.at[axis, 2],
            peer(tp=nears[axis]),
        )

    for order in range(2):
        for axis in range(2):
            outward(axis, (1 - axis + order) % 2).start()
    own = pltpu.make_async_copy(
        block, whole.at[:, pl.ds(pl.multiple_of(tp * width, width), width)], own_sem
    )
    own.start()
    for axis in range(2):
        inward(1 - axis, axis).wait_recv()
        relay(axis).start()
    for axis in range(2):
        inward(axis, 1 - (1 - axis)).wait_recv()
        relayed(axis).wait_recv()
        relay(axis).wait_send()
        for part in range(2):
            outward(axis, part).wait_send()
    own.wait()


def any_space(count):
    return [pl.BlockSpec(memory_space=pl.ANY)] * count


def vmem_space(count):
    return [pl.BlockSpec(memory_space=pltpu.VMEM)] * count


def gather_features(block, number):
    rows, width = block.shape
    return pl.pallas_call(
        gather_kernel,
        name=f"gather_{number}",
        out_shape=jax.ShapeDtypeStruct((rows, 4 * width), block.dtype),
        in_specs=vmem_space(1),
        out_specs=pl.BlockSpec(memory_space=pl.ANY),
        scratch_shapes=[
            pltpu.SemaphoreType.DMA((2, 3)),
            pltpu.SemaphoreType.DMA((2, 3)),
            pltpu.SemaphoreType.DMA,
        ],
        compiler_params=pltpu.CompilerParams(collective_id=number, has_side_effects=True),
    )(block)


def dispatch_kernel(
    n_sp, rows, mid, down, rows_all, mid_all, down_all, z_send, z_recv, t_send, t_recv, own_sem
):
    me = lax.axis_index("sp")
    tp = lax.axis_index("tp")
    width = mid.shape[1]
    for d in range(1, n_sp):
        greet(peer(sp=(me + d) % n_sp))
    for d in range(1, 4):
        greet(peer(tp=(tp + d) % 4))
    pl.semaphore_wait(pltpu.get_barrier_semaphore(), n_sp - 1 + 3)

    def columns(owner):
        return mid_all.at[:, pl.ds(pl.multiple_of(owner * width, width), width)]

    def row_copy(d):
        to = (me + d) % n_sp
        return send(rows.at[to], rows_all.at[me], z_send.at[d], z_recv.at[d], peer(sp=to))

    def row_arrival(d):
        source = (me - d + n_sp) % n_sp
        return send(rows.at[source], rows_all.at[source], z_send.at[d], z_recv.at[d], peer(sp=source))

    half = down.shape[1] // 2

    def side_copies(d):
        to = (tp + d) % 4
        return [send(mid, columns(tp), t_send.at[d, 0], t_recv.at[d, 0], peer(tp=to))] + [
            send(
                down.at[to, pl.ds(i * half, half)],
                down_all.at[tp, pl.ds(i * half, half)],
                t_send.at[d, 1 + i],
                t_recv.at[d, 1 + i],
                peer(tp=to),
            )
            for i in range(2)
        ]

    def side_arrivals(d):
        source = (tp - d + 4) % 4
        return [send(mid, columns(source), t_send.at[d, 0], t_recv.at[d, 0], peer(tp=source))] + [
            send(
                down.at[source, pl.ds(i * half, half)],
                down_all.at[source, pl.ds(i * half, half)],
                t_send.at[d, 1 + i],
                t_recv.at[d, 1 + i],
                peer(tp=source),
            )
            for i in range(2)
        ]

    middle = n_sp // 2
    groups = [side_copies(d) for d in (2, 1, 3)]
    sides = [group[i] for i in range(3) for group in groups]
    straight = [row_copy(d) for d in sorted(range(1, n_sp), key=lambda d: abs(d - middle))]
    for i in range(max(len(sides), len(straight))):
        if i < len(straight):
            straight[i].start()
        if i < len(sides):
            sides[i].start()
    own = (
        pltpu.make_async_copy(rows.at[me], rows_all.at[me], own_sem.at[0]),
        pltpu.make_async_copy(mid, columns(tp), own_sem.at[1]),
    )
    for copy in own:
        copy.start()
    for d in range(1, n_sp):
        row_arrival(d).wait_recv()
        row_copy(d).wait_send()
    for d in range(1, 4):
        for copy in side_arrivals(d):
            copy.wait_recv()
        for copy in side_copies(d):
            copy.wait_send()
    for copy in own:
        copy.wait()


def return_kernel(n_sp, produced, final, stage, t_send, t_recv, z_send, z_recv, own_sem):
    me = lax.axis_index("sp")
    tp = lax.axis_index("tp")
    for d in range(1, n_sp):
        greet(peer(sp=(me + d) % n_sp))
    for d in range(1, 4):
        greet(peer(tp=(tp + d) % 4))
    pl.semaphore_wait(pltpu.get_barrier_semaphore(), n_sp - 1 + 3)

    def target(d):
        return (me + d) % n_sp

    def landing(d, owner):
        return final.at[me, owner] if d == 0 else stage.at[target(d), owner]

    def side_copy(d, r):
        to = (tp + r) % 4
        return send(
            produced.at[to, target(d)], landing(d, tp), t_send.at[d, r], t_recv.at[d, r], peer(tp=to)
        )

    def side_arrival(d, r):
        source = (tp - r + 4) % 4
        return send(
            produced.at[source, target(d)],
            landing(d, source),
            t_send.at[d, r],
            t_recv.at[d, r],
            peer(tp=source),
        )

    def back_copy(d, r):
        owner = (tp - r + 4) % 4
        src = produced.at[tp, target(d)] if r == 0 else stage.at[target(d), owner]
        return send(
            src, final.at[me, owner], z_send.at[d, r], z_recv.at[d, r], peer(sp=target(d))
        )

    def back_arrival(d, r):
        owner = (tp - r + 4) % 4
        source = (me - d + n_sp) % n_sp
        return send(
            produced.at[tp, source],
            final.at[source, owner],
            z_send.at[d, r],
            z_recv.at[d, r],
            peer(sp=source),
        )

    half = n_sp // 2
    order = sorted(range(1, n_sp), key=lambda d: abs(d - half))
    for d in order:
        back_copy(d, 0).start()
    for d in order + [0]:
        for r in (2, 1, 3):
            side_copy(d, r).start()
    own = pltpu.make_async_copy(produced.at[tp, me], final.at[me, tp], own_sem)
    own.start()
    for d in order:
        for r in (1, 3, 2):
            side_arrival(d, r).wait_recv()
            back_copy(d, r).start()
    for r in range(1, 4):
        side_arrival(0, r).wait_recv()
    for d in range(n_sp):
        for r in range(1, 4):
            side_copy(d, r).wait_send()
    for d in order:
        for r in range(4):
            back_arrival(d, r).wait_recv()
            back_copy(d, r).wait_send()
    own.wait()


def attention_kernel(q_ref, k_ref, v_ref, g_ref, o_ref, top, total, summed):
    me = lax.axis_index("sp")
    heads = g_ref.shape[1]
    rows = q_ref.shape[0]
    dim = q_ref.shape[1] // heads
    for h in range(heads):
        top[h] = jnp.full(top.shape[1:], -1e30, jnp.float32)
        total[h] = jnp.zeros(total.shape[1:], jnp.float32)
        summed[h] = jnp.zeros(summed.shape[1:], jnp.float32)

    def fold(j, masked):
        for h in range(heads):
            columns = slice(h * dim, (h + 1) * dim)
            scores = lax.dot_general(
                q_ref[:, columns],
                k_ref[j, :, columns],
                (((1,), (1,)), ((), ())),
                preferred_element_type=jnp.float32,
            )
            scores = scores - g_ref[j, h : h + 1, :]
            if masked:
                row = lax.broadcasted_iota(jnp.int32, scores.shape, 0)
                column = lax.broadcasted_iota(jnp.int32, scores.shape, 1)
                scores = jnp.where(column <= row, scores, -jnp.inf)
            old = top[h]
            new = jnp.maximum(old, jnp.max(scores, axis=1, keepdims=True))
            factor = jnp.exp(old - new)
            weight = jnp.exp(scores - new)
            total[h] = total[h] * factor + jnp.sum(weight, axis=1, keepdims=True)
            summed[h] = summed[h] * factor + jnp.dot(
                weight.astype(jnp.bfloat16), v_ref[j, :, columns], preferred_element_type=jnp.float32
            )
            top[h] = new

    def one(j, carry):
        fold(j, False)
        return carry

    lax.fori_loop(0, me, one, 0)
    fold(me, True)
    for h in range(heads):
        o_ref[:, h * dim : (h + 1) * dim] = (summed[h] / total[h]).astype(o_ref.dtype)


def expert_kernel(
    rows, gate_own, up_own, down_own, gate_all, up_all, down_all, produced, gate, up, down, sems
):
    tp = lax.axis_index("tp")
    owns, wholes, targets = (gate_own, up_own, down_own), (gate_all, up_all, down_all), (gate, up, down)
    copies = []
    for i in range(3):
        width = owns[i].shape[2]
        for d in range(4):
            source = (tp + d) % 4
            src = owns[i].at[tp] if d == 0 else wholes[i].at[source]
            columns = pl.ds(pl.multiple_of(source * width, width), width)
            copies.append(pltpu.make_async_copy(src, targets[i].at[:, columns], sems.at[i, d]))
            copies[-1].start()
    for copy in copies[:4]:
        copy.wait()
    gate_part = jnp.dot(rows[...], gate[...], preferred_element_type=jnp.float32)
    for copy in copies[4:8]:
        copy.wait()
    up_part = jnp.dot(rows[...], up[...], preferred_element_type=jnp.float32)
    hidden = silu_gate(gate_part, up_part).astype(jnp.bfloat16)
    for copy in copies[8:]:
        copy.wait()
    width = produced.shape[2]
    for t in range(4):
        produced[t] = jnp.dot(
            hidden, down[:, t * width : (t + 1) * width], preferred_element_type=jnp.float32
        ).astype(produced.dtype)


def fast_shards(
    queries,
    key_vectors,
    value_vectors,
    log_gate_sums,
    residual,
    out_weight,
    norm_gain,
    routes,
    route_weight,
    expert_gate,
    expert_up,
    expert_down,
    shared_gate,
    shared_up,
    shared_down,
):
    n_sp = lax.axis_size("sp")
    tp = lax.axis_index("tp")
    tok_dev = queries.shape[0]
    heads = log_gate_sums.shape[1]
    local_width = residual.shape[1]
    model_width = norm_gain.shape[0]
    exp_dev = expert_gate.shape[0]
    experts_all = exp_dev * n_sp
    top_count = routes.shape[1]
    capacity = 5 * tok_dev * top_count // (4 * experts_all)
    depth = n_sp // 2

    def like(shape, array):
        return jax.ShapeDtypeStruct(shape, array.dtype)

    gates = log_gate_sums.T
    k_all, v_all, g_all, gate_all, up_all = pl.pallas_call(
        functools.partial(kv_kernel, n_sp),
        name="kv_share",
        out_shape=(
            like((n_sp,) + key_vectors.shape, key_vectors),
            like((n_sp,) + value_vectors.shape, value_vectors),
            like((n_sp,) + gates.shape, gates),
            like(expert_gate.shape, expert_gate),
            like(expert_up.shape, expert_up),
        ),
        in_specs=vmem_space(3) + any_space(2),
        out_specs=tuple(any_space(5)),
        scratch_shapes=[
            pltpu.SemaphoreType.DMA((depth, 3)),
            pltpu.SemaphoreType.DMA((depth, 3)),
            pltpu.SemaphoreType.DMA((depth, 3)),
            pltpu.SemaphoreType.DMA((depth, 3)),
            pltpu.SemaphoreType.DMA((3, 2)),
            pltpu.SemaphoreType.DMA((3, 2)),
            pltpu.SemaphoreType.DMA((3,)),
        ],
        compiler_params=pltpu.CompilerParams(collective_id=1, has_side_effects=True),
    )(key_vectors, value_vectors, gates, expert_gate, expert_up)

    scaled = (queries.astype(jnp.float32) * HDIM ** (-0.5)).astype(jnp.bfloat16)
    attended = pl.pallas_call(
        attention_kernel,
        name="attention",
        out_shape=like(queries.shape, queries),
        in_specs=vmem_space(4),
        out_specs=pl.BlockSpec(memory_space=pltpu.VMEM),
        scratch_shapes=[
            pltpu.VMEM((heads, tok_dev, 1), jnp.float32),
            pltpu.VMEM((heads, tok_dev, 1), jnp.float32),
            pltpu.VMEM((heads, tok_dev, HDIM), jnp.float32),
        ],
        compiler_params=pltpu.CompilerParams(vmem_limit_bytes=40 * 1024 * 1024),
    )(scaled, k_all, v_all, g_all)

    flat_routes = routes.reshape(-1)
    onehot = flat_routes[:, None] == jnp.arange(experts_all, dtype=jnp.int32)[None, :]
    pairs = tok_dev * top_count
    earlier = (
        jnp.arange(pairs, dtype=jnp.int32)[None, :] < jnp.arange(pairs, dtype=jnp.int32)[:, None]
    ).astype(jnp.bfloat16)
    before = jnp.dot(earlier, onehot.astype(jnp.bfloat16), preferred_element_type=jnp.float32)
    rank = jnp.sum(jnp.where(onehot, before, 0.0), axis=1).astype(jnp.int32)
    rank = rank.reshape(tok_dev, top_count)
    targets = routes * capacity + rank
    here = jnp.where(routes % exp_dev == tp, routes // exp_dev * capacity + rank, -1)
    slots = jnp.arange(n_sp * capacity, dtype=jnp.int32)[:, None]
    chosen = slots == here[:, 0][None, :]
    for k in range(1, top_count):
        chosen = chosen | (slots == here[:, k][None, :])
    chosen = chosen.astype(jnp.bfloat16)

    attended_all = gather_features(attended, 2)
    projected = jnp.dot(attended_all, out_weight, preferred_element_type=jnp.float32)
    mid = (residual.astype(jnp.float32) + projected).astype(jnp.bfloat16)
    mid_all = gather_features(mid, 3).astype(jnp.float32)
    inverse = lax.rsqrt(jnp.mean(mid_all * mid_all, axis=1, keepdims=True) + EPSILON)
    normed = (mid_all * inverse * norm_gain.astype(jnp.float32)[None, :]).astype(jnp.bfloat16)
    rows = jnp.dot(chosen, normed, preferred_element_type=jnp.float32).astype(jnp.bfloat16)
    rows = rows.reshape(n_sp, capacity, model_width)
    shared_mid = silu_gate(
        jnp.dot(normed, shared_gate, preferred_element_type=jnp.float32),
        jnp.dot(normed, shared_up, preferred_element_type=jnp.float32),
    ).astype(jnp.bfloat16)

    rows_all, shared_all, down_all = pl.pallas_call(
        functools.partial(dispatch_kernel, n_sp),
        name="dispatch",
        out_shape=(
            like(rows.shape, rows),
            like((tok_dev, 4 * shared_mid.shape[1]), shared_mid),
            like(expert_down.shape, expert_down),
        ),
        in_specs=vmem_space(2) + any_space(1),
        out_specs=tuple(any_space(3)),
        scratch_shapes=[
            pltpu.SemaphoreType.DMA((n_sp,)),
            pltpu.SemaphoreType.DMA((n_sp,)),
            pltpu.SemaphoreType.DMA((4, 3)),
            pltpu.SemaphoreType.DMA((4, 3)),
            pltpu.SemaphoreType.DMA((2,)),
        ],
        compiler_params=pltpu.CompilerParams(collective_id=4, has_side_effects=True),
    )(rows, shared_mid, expert_down)

    produced = pl.pallas_call(
        expert_kernel,
        name="experts",
        out_shape=like((4, n_sp * capacity, local_width), rows),
        in_specs=vmem_space(1) + any_space(6),
        out_specs=pl.BlockSpec(memory_space=pltpu.VMEM),
        scratch_shapes=[
            pltpu.VMEM((model_width, 4 * expert_gate.shape[2]), jnp.bfloat16),
            pltpu.VMEM((model_width, 4 * expert_up.shape[2]), jnp.bfloat16),
            pltpu.VMEM((expert_down.shape[1], 4 * expert_down.shape[2]), jnp.bfloat16),
            pltpu.SemaphoreType.DMA((3, 4)),
        ],
        compiler_params=pltpu.CompilerParams(vmem_limit_bytes=40 * 1024 * 1024),
    )(
        rows_all.reshape(n_sp * capacity, model_width),
        expert_gate,
        expert_up,
        expert_down,
        gate_all,
        up_all,
        down_all,
    ).reshape(4, n_sp, capacity, local_width)

    final = pl.pallas_call(
        functools.partial(return_kernel, n_sp),
        name="give_back",
        out_shape=like((n_sp, 4, capacity, local_width), produced),
        in_specs=vmem_space(1),
        out_specs=pl.BlockSpec(memory_space=pl.ANY),
        scratch_shapes=[
            pltpu.VMEM((n_sp, 4, capacity, local_width), jnp.bfloat16),
            pltpu.SemaphoreType.DMA((n_sp, 4)),
            pltpu.SemaphoreType.DMA((n_sp, 4)),
            pltpu.SemaphoreType.DMA((n_sp, 4)),
            pltpu.SemaphoreType.DMA((n_sp, 4)),
            pltpu.SemaphoreType.DMA,
        ],
        compiler_params=pltpu.CompilerParams(collective_id=5, has_side_effects=True),
    )(produced)

    shared_out = jnp.dot(shared_all, shared_down, preferred_element_type=jnp.float32)
    returned = final.reshape(experts_all * capacity, local_width)
    places = jnp.arange(experts_all * capacity, dtype=jnp.int32)[None, :]
    result = mid.astype(jnp.float32) + shared_out
    for k in range(top_count):
        pick = (places == targets[:, k][:, None]).astype(jnp.bfloat16)
        picked = jnp.dot(pick, returned, preferred_element_type=jnp.float32)
        result = result + picked * route_weight[:, k][:, None]
    return result.astype(jnp.bfloat16)


def solution(mesh):
    placed = (
        P("sp", "tp"),
        P("sp", "tp"),
        P("sp", "tp"),
        P("sp", "tp"),
        P("sp", "tp"),
        P(None, "tp"),
        P(),
        P("sp", None),
        P("sp", None),
        P("sp", None, "tp"),
        P("sp", None, "tp"),
        P("sp", None, "tp"),
        P(None, "tp"),
        P(None, "tp"),
        P(None, "tp"),
    )
    fits = mesh.shape["tp"] == 4 and mesh.shape["sp"] % 2 == 0 and mesh.shape["sp"] <= 16
    return jax.shard_map(
        fast_shards if fits else shards, mesh=mesh, in_specs=placed, out_specs=P("sp", "tp"), check_vma=False
    )
```
